32 devices in a mesh: rep: 2 (over x), fs: 4 (over z), tp: 4 (over y, core).
Axes of the slice: x: 2, y: 2, z: 4, core: 2. Of those that a mesh axis runs over, the one named last changes fastest.
Arguments:
- tokens: bfloat16 [8192, 1024], P(('rep', 'fs', 'tp')), may hold values from -6 to 6
- norm_gain: float32 [1024], replicated, may hold values from 0.5 to 1.5
- gate_weight: bfloat16 [1024, 3072], P(('rep', 'fs'), 'tp'), may hold values from -0.1875 to 0.1875
- up_weight: bfloat16 [1024, 3072], P(('rep', 'fs'), 'tp'), may hold values from -0.1875 to 0.1875
- down_weight: bfloat16 [3072, 1024], P('tp', ('rep', 'fs')), may hold values from -0.109375 to 0.109375
Outputs:
- block_out: bfloat16 [8192, 1024], P(('rep', 'fs', 'tp'))
The draws below stay inside these ranges and needn't reach their ends.
All inputs are finite; a program needn't handle non-finite values.
Results may differ from the reference program's by a relative error of at most 0.001.
Values may be sent and summed in bfloat16 or wider, within the bound.
A program may use at most 64 MiB of HBM per device.

```python
import jax
import jax.numpy as jnp
from jax import lax

D = 1024
FF = 3072
TOKENS = 8192


def level_of(rng, extent, shards, smallest, largest):
    loudness, own = 1.0, jax.random.fold_in(rng, 6)
    for position, parts in shards:
        steps = jnp.exp(jax.random.uniform(jax.random.fold_in(own, position), (parts,), jnp.float32, smallest / len(shards), largest / len(shards)))
        loudness = loudness * jnp.repeat(steps, extent[position] // parts).reshape([-1 if axis == position else 1 for axis in range(len(extent))])
    return loudness


def noise(rng, dims, spread, most, cuts=(), held_as=jnp.bfloat16):
    gain = level_of(rng, dims, cuts, -0.22, 0.18) if cuts else 1.0
    result = jax.random.normal(rng, dims, jnp.float32) * spread * gain
    return jnp.minimum(jnp.maximum(result, -most), most).astype(held_as)


def setup_inputs(seed: int = 0) -> dict:
    streams_of = jax.random.split(jax.random.key(seed), 6)
    tokens = noise(streams_of[0], (TOKENS, D), 1.0, 6.0, ((0, 32),))
    norm_gain = jnp.clip(1.0 + 0.1 * jax.random.normal(streams_of[1], (D,), jnp.float32), 0.5, 1.5)
    gate_weight = noise(streams_of[2], (D, FF), D ** -0.5, 0.1875, ((0, 8), (1, 4)))
    up_weight = noise(streams_of[3], (D, FF), D ** -0.5, 0.1875, ((0, 8), (1, 4)))
    down_weight = noise(streams_of[4], (FF, D), FF ** -0.5, 0.109375, ((0, 4), (1, 8)))
    return dict(tokens=tokens, norm_gain=norm_gain, gate_weight=gate_weight, up_weight=up_weight, down_weight=down_weight)


epsilon = 1e-06

def reference(tokens, norm_gain, gate_weight, up_weight, down_weight):
    values = tokens.astype(jnp.float32)
    inverse_rms = lax.rsqrt(lax.optimization_barrier(jnp.mean(values * values, axis=-1, keepdims=True)) + epsilon)
    normed = (values * inverse_rms * norm_gain.astype(jnp.float32)).astype(jnp.bfloat16)
    gate_value = jnp.dot(normed, gate_weight, preferred_element_type=jnp.float32)
    up_value = jnp.dot(normed, up_weight, preferred_element_type=jnp.float32)
    hidden = (jax.nn.silu(gate_value) * up_value).astype(jnp.bfloat16)
    return jnp.dot(hidden, down_weight, preferred_element_type=jnp.float32).astype(jnp.bfloat16)
```

```python
import functools

import jax
import jax.numpy as jnp
from jax import lax
from jax.experimental import pallas as pl
from jax.experimental.pallas import tpu as pltpu
from jax.sharding import PartitionSpec as P

epsilon = 1e-06
MESH = pl.DeviceIdType.MESH


def over_all(shard, axis, dim, absorb, carry):
    whole = jax.tree.map(lambda part: lax.all_gather(part, axis, axis=dim, tiled=True), shard)
    return absorb(carry, whole, jnp.int32(0))


def summed_rows(portion, width, axis):
    count = width * lax.axis_size(axis)
    return lax.psum_scatter(portion(jnp.int32(0), count), axis, scatter_dimension=0, tiled=True)


def on_device(tokens, norm_gain, gate_weight, up_weight, down_weight):
    values = tokens.astype(jnp.float32)
    inverse_rms = lax.rsqrt(jnp.mean(values * values, axis=-1, keepdims=True) + epsilon)
    normed = (values * inverse_rms * norm_gain.astype(jnp.float32)).astype(jnp.bfloat16)
    gathered = lax.all_gather(normed, "tp", axis=0, tiled=True)
    zero_sums = jnp.zeros((gathered.shape[0], gate_weight.shape[1]), jnp.float32)

    def add_block(running, row_block, first_row):
        columns = lax.dynamic_slice_in_dim(gathered, first_row, row_block.shape[0], 1)
        return running + jnp.dot(columns, row_block, preferred_element_type=jnp.float32)

    gate_value = over_all(gate_weight, ("rep", "fs"), 0, add_block, zero_sums)
    up_value = over_all(up_weight, ("rep", "fs"), 0, add_block, zero_sums)
    hidden = (jax.nn.silu(gate_value) * up_value).astype(jnp.bfloat16)
    own_half = lax.all_gather(down_weight, "fs", axis=1, tiled=True)
    down_whole = lax.all_gather(own_half, "rep", axis=1, tiled=True)
    own_rows = tokens.shape[0]

    def row_terms(first_row, row_count):
        token_block = lax.dynamic_slice_in_dim(hidden, first_row, row_count, 0)
        return jnp.dot(token_block, down_whole, preferred_element_type=jnp.float32)

    mixed_out = summed_rows(row_terms, own_rows, "tp")
    return mixed_out.astype(jnp.bfloat16)


def kernel(
    fs_size, tok_ref, gain_ref, g_ref, u_ref, d_ref, out_ref,
    gbuf, ubuf, dbuf, tokbuf, xn, gacc, uacc, hid, psend, precv, pkeep,
    ring_send, ring_recv, pair_send, pair_recv, peer_send, peer_recv, tok_sem,
):
    n = 2 * fs_size
    half = n // 2
    rows, width = tok_ref.shape
    depth, cols = g_ref.shape
    out_cols = d_ref.shape[1]
    tile = 256

    rep, fs, tp = lax.axis_index("rep"), lax.axis_index("fs"), lax.axis_index("tp")
    place = fs + rep * (n - 1 - 2 * fs)

    def at_place(q):
        rep_q = q // fs_size
        return rep_q, q + rep_q * (n - 1 - 2 * q)

    def device_at(q):
        rep_q, fs_q = at_place(q)
        return {"rep": rep_q, "fs": fs_q, "tp": tp}

    def block_of(slot):
        rep_q, fs_q = at_place((place + n - slot) % n)
        return rep_q * fs_size + fs_q

    right, left = device_at((place + 1) % n), device_at((place + n - 1) % n)
    partner = {"rep": rep, "fs": fs, "tp": tp + 1 - 2 * (tp % 2)}
    peer = {"rep": rep, "fs": fs, "tp": (tp + 2) % 4}

    own, buf = (g_ref, u_ref, d_ref), (gbuf, ubuf, dbuf)

    def held(kind, side, slot):
        return own[kind] if side == 0 and slot == 0 else buf[kind].at[side, slot]

    def ring(kind, way, slot):
        to = slot + 1 if way == 0 else (slot - 1) % n
        src, dst = held(kind, 0, slot), buf[kind].at[0, to]
        if kind == 2 and to == half:
            part = pl.ds(way * (cols // 2), cols // 2)
            src, dst = src.at[part], dst.at[part]
        return pltpu.make_async_remote_copy(
            src_ref=src, dst_ref=dst,
            send_sem=ring_send.at[way, kind, slot], recv_sem=ring_recv.at[way, kind, to],
            device_id=right if way == 0 else left, device_id_type=MESH,
        )

    def pair(kind, slot):
        return pltpu.make_async_remote_copy(
            src_ref=held(kind, 0, slot), dst_ref=buf[kind].at[1, slot],
            send_sem=pair_send.at[kind, slot], recv_sem=pair_recv.at[kind, slot],
            device_id=partner, device_id_type=MESH,
        )

    def out_copy(slot):
        return pltpu.make_async_remote_copy(
            src_ref=psend.at[slot], dst_ref=precv.at[slot],
            send_sem=peer_send.at[slot], recv_sem=peer_recv.at[slot],
            device_id=peer, device_id_type=MESH,
        )

    tok_copy = pltpu.make_async_remote_copy(
        src_ref=tok_ref, dst_ref=tokbuf, send_sem=tok_sem.at[0], recv_sem=tok_sem.at[1],
        device_id=peer, device_id_type=MESH,
    )
    sent = []

    def start(copy):
        copy.start()
        sent.append(copy)

    barrier = pltpu.get_barrier_semaphore()
    for device in (left, right, partner, peer):
        pl.semaphore_signal(barrier, inc=1, device_id=device, device_id_type=MESH)
    pl.semaphore_wait(barrier, 4)

    for kind in (0, 1):
        for way in (0, 1):
            start(ring(kind, way, 0))
    start(tok_copy)
    for kind in (0, 1, 2):
        start(pair(kind, 0))

    def arrive(kind, k):
        for way in (0, 1):
            last = kind < 2 and k == half - 1 and way != kind
            slot = k if way == 0 else n - k
            ring(kind, way, (slot - 1) if way == 0 else (slot + 1) % n).wait_recv()
            if not last:
                start(ring(kind, way, slot))
            start(pair(kind, slot))

    def normalize(ref, first):
        step = 32

        @pl.loop(0, rows // step)
        def _(i):
            values = ref[pl.ds(pl.multiple_of(i * step, step), step), :].astype(jnp.float32)
            scale = lax.rsqrt(jnp.mean(values * values, axis=-1, keepdims=True) + epsilon)
            normed = (values * scale * gain_ref[...]).astype(jnp.bfloat16)
            where = pl.ds(pl.multiple_of(first + i * step, step), step)
            for b in range(n):
                xn[b, where, :] = normed[:, b * depth:(b + 1) * depth]

    def project(kind, k):
        acc = (gacc, uacc)[kind]
        a, b = (k, n - k) if k else (0, half)
        lhs_a, lhs_b = block_of(a), block_of(b)
        for side in (0, 1):
            for slot in (a, b):
                if side == 1:
                    pair(kind, slot).wait_recv()

            @pl.loop(0, cols // tile)
            def _(i):
                cut = pl.ds(pl.multiple_of(i * tile, tile), tile)
                lhs = jnp.concatenate([xn[lhs_a], xn[lhs_b]], axis=1)
                rhs = jnp.concatenate([held(kind, side, a)[:, cut], held(kind, side, b)[:, cut]], axis=0)
                part = jnp.dot(lhs, rhs, preferred_element_type=jnp.float32)
                to = pl.ds(pl.multiple_of(side * cols + i * tile, tile), tile)
                if k == 1:
                    acc[:, to] = part
                else:
                    acc[:, to] += part

    def down(slots):
        for slot in slots:
            pair(2, slot).wait_recv()
        rhs = jnp.concatenate(
            [jnp.concatenate([held(2, side, slot)[...] for side in (0, 1)], axis=0) for slot in slots], axis=1
        )
        for first, store in ((0, psend), (rows, pkeep)):
            part = jnp.dot(hid[first:first + rows, :], rhs, preferred_element_type=jnp.float32)
            for j, slot in enumerate(slots):
                store[slot] = part[:, j * out_cols:(j + 1) * out_cols]
        for slot in slots:
            start(out_copy(slot))

    normalize(tok_ref, rows)
    arrive(0, 1)
    arrive(1, 1)
    tok_copy.wait_recv()
    normalize(tokbuf, 0)
    project(0, 1)
    for k in range(2, half):
        arrive(0, k)
        project(1, k - 1)
        arrive(1, k)
        project(0, k)
    start(ring(2, 0, 0))
    start(ring(2, 1, 0))
    project(1, half - 1)
    ring(0, 0, half - 1).wait_recv()
    start(pair(0, half))
    ring(1, 1, half + 1).wait_recv()
    start(pair(1, half))
    project(0, 0)
    project(1, 0)

    @pl.loop(0, 2 * rows // 16)
    def _(i):
        where = pl.ds(pl.multiple_of(i * 16, 16), 16)
        gate = gacc[where, :]
        hid[where, :] = (gate / (1.0 + jnp.exp(-gate)) * uacc[where, :]).astype(jnp.bfloat16)

    down((0,))
    for k in range(1, half):
        arrive(2, k)
        down((k, n - k))
    ring(2, 0, half - 1).wait_recv()
    ring(2, 1, half + 1).wait_recv()
    start(pair(2, half))
    down((half,))

    order = [0] + [s for k in range(1, half) for s in (k, n - k)] + [half]
    for slot in order:
        out_copy(slot).wait_recv()
        to = pl.ds(pl.multiple_of(block_of(slot) * out_cols, out_cols), out_cols)
        out_ref[:, to] = (pkeep[slot] + precv[slot]).astype(out_ref.dtype)
    for copy in sent:
        copy.wait_send()


def fused(fs_size, tokens, norm_gain, gate_weight, up_weight, down_weight):
    n = 2 * fs_size
    rows, width = tokens.shape
    depth, cols = gate_weight.shape
    out_cols = down_weight.shape[1]
    vmem = pl.BlockSpec(memory_space=pltpu.VMEM)
    bf16, f32 = jnp.bfloat16, jnp.float32
    dma = pltpu.SemaphoreType.DMA
    return pl.pallas_call(
        functools.partial(kernel, fs_size),
        out_shape=jax.ShapeDtypeStruct((rows, width), bf16),
        in_specs=[vmem] * 5,
        out_specs=vmem,
        scratch_shapes=[
            pltpu.VMEM((2, n, depth, cols), bf16),
            pltpu.VMEM((2, n, depth, cols), bf16),
            pltpu.VMEM((2, n, cols, out_cols), bf16),
            pltpu.VMEM((rows, width), bf16),
            pltpu.VMEM((n, 2 * rows, depth), bf16),
            pltpu.VMEM((2 * rows, 2 * cols), f32),
            pltpu.VMEM((2 * rows, 2 * cols), f32),
            pltpu.VMEM((2 * rows, 2 * cols), bf16),
            pltpu.VMEM((n, rows, out_cols), f32),
            pltpu.VMEM((n, rows, out_cols), f32),
            pltpu.VMEM((n, rows, out_cols), f32),
            dma((2, 3, n)),
            dma((2, 3, n)),
            dma((3, n)),
            dma((3, n)),
            dma((n,)),
            dma((n,)),
            dma((2,)),
        ],
        compiler_params=pltpu.CompilerParams(
            collective_id=0, has_side_effects=True, vmem_limit_bytes=60 * 1024 * 1024
        ),
    )(tokens, norm_gain.astype(f32).reshape(1, width), gate_weight, up_weight, down_weight)


def solution(mesh):
    sizes = dict(mesh.shape)

    def run(tokens, norm_gain, gate_weight, up_weight, down_weight):
        covered = (
            sizes["rep"] == 2 and sizes["tp"] == 4 and sizes["fs"] >= 2
            and gate_weight.shape[0] % 128 == 0 and gate_weight.shape[1] % 256 == 0
            and down_weight.shape[1] % 128 == 0 and tokens.shape[0] % 32 == 0
        )
        body = functools.partial(fused, sizes["fs"]) if covered else on_device
        return body(tokens, norm_gain, gate_weight, up_weight, down_weight)

    return jax.shard_map(
        run,
        mesh=mesh,
        in_specs=(
            P(("rep", "fs", "tp"), None),
            P(),
            P(("rep", "fs"), "tp"),
            P(("rep", "fs"), "tp"),
            P("tp", ("rep", "fs")),
        ),
        out_specs=P(("rep", "fs", "tp"), None),
        check_vma=False,
    )
```
